32 devices in a mesh: sp: 8 (over z, y), tp: 4 (over x, core).
Axes of the slice: x: 2, y: 2, z: 4, core: 2. Of those that a mesh axis runs over, the one named last changes fastest.
Arguments:
- queries: bfloat16 [2048, 1024], P('sp', 'tp'), may hold values from -8 to 8
- keys: bfloat16 [2048, 256], P('sp', 'tp'), may hold values from -6 to 6
- values: bfloat16 [2048, 256], P('sp', 'tp'), may hold values from -6 to 6
- query_gain: float32 [64], replicated, may hold values from 0.3 to 9
- key_norm_gain: float32 [64], replicated, may hold values from 0.3 to 9
- attn_gain: float32 [1024], replicated, may hold values from 0.1 to 1.9
- residual: bfloat16 [2048, 2048], P('sp', 'tp'), may hold values from -20 to 20
- out_weight: bfloat16 [1024, 2048], P(None, 'tp'), may hold values from -0.1875 to 0.1875
- ffn_gain: float32 [2048], P('tp'), may hold values from 0.1 to 1.9
- routes: int32 [2048, 4], P('sp'), may hold values from 0 to 7, all different within a row; in each aligned block of 256 rows (0 to 255, 256 to 511, ...) at most 192 rows name the same one
- route_weight: float32 [2048, 4], P('sp'), may hold values from 0.2 to 1
- gate_weight: bfloat16 [8, 2048, 2048], P('sp', None, 'tp'), may hold values from -0.5 to 0.5
- up_weight: bfloat16 [8, 2048, 2048], P('sp', None, 'tp'), may hold values from -0.5 to 0.5
- down_weight: bfloat16 [8, 2048, 2048], P('sp', 'tp'), may hold values from -0.0068359375 to 0.0068359375
Outputs:
- layer_out: bfloat16 [2048, 2048], P('sp', 'tp')
The draws below stay inside these ranges and needn't reach their ends.
Inputs may be any that keep to these rules, and one draw needn't show every extreme that they name: Each token names 4 different experts. In the tokens of one index of sp (aligned blocks of 256 tokens) no expert is named by more than 192 routes, a bound that some block reaches.
All inputs are finite; a program needn't handle non-finite values.
Results may differ from the reference program's by a relative error of at most 0.012.
The reference program's roundings to bfloat16 on the way count: a program that leaves them out, or rounds other values in their place, can miss the bound.
Values may be sent and summed in bfloat16 or wider, within the bound.
No kernel may reach another device: no remote copies, remote signals or barrier semaphores. Data moves between devices by JAX's collectives and lax.ppermute only.
A program may use at most 64 MiB of HBM per device.

```python
import math
import jax
import jax.numpy as jnp
import numpy as np
from jax import lax

D = 2048
FF = 2048
HEAD_DIMENSION = 64
QUERY_HEADS = 16
KEY_VALUE_HEADS = 4
TOPK = 4
GRID_W = 64
TOK_SP = 256
SEQUENCE_TOKENS = 2048
EXPERTS = 8
CAP = 192
N_SP = 8
N_TP = 4


def gain_values(key, salt_value):
    noise_sample = jax.random.uniform(jax.random.fold_in(key, salt_value), (HEAD_DIMENSION,), jnp.float32)
    return 0.5 + noise_sample


def draw_query_gain(key, part):
    return gain_values(key, 502)


def draw_key_norm_gain(key, part):
    return gain_values(key, 503)


def key_head_rows(key):
    baseline_sample = jax.random.normal(jax.random.fold_in(key, 601), (SEQUENCE_TOKENS, KEY_VALUE_HEADS, HEAD_DIMENSION), jnp.float32)
    return jnp.clip(baseline_sample, -6.0, 6.0)


def draw_keys(key, part):
    return key_head_rows(key).reshape(SEQUENCE_TOKENS, KEY_VALUE_HEADS * HEAD_DIMENSION).astype(jnp.bfloat16)


def draw_queries(key, part):
    group_width = QUERY_HEADS // KEY_VALUE_HEADS
    noise_sample = jax.random.normal(jax.random.fold_in(key, 602), (SEQUENCE_TOKENS, KEY_VALUE_HEADS, group_width, HEAD_DIMENSION), jnp.float32)
    return jnp.clip(noise_sample, -8.0, 8.0).reshape(SEQUENCE_TOKENS, QUERY_HEADS * HEAD_DIMENSION).astype(jnp.bfloat16)


def draw_residual(key, part):
    columns = jnp.arange(D, dtype=jnp.float32) / D
    baseline_sample = jnp.clip(jax.random.normal(jax.random.fold_in(key, 701), (SEQUENCE_TOKENS, D), jnp.float32), -6.0, 6.0)
    column_scale = 0.6 * jnp.exp(jnp.log(5.0) * columns)
    return (baseline_sample * column_scale[None, :]).astype(jnp.bfloat16)


def level_of(own_key, shape, cuts, low, high):
    def one(position, blocks):
        steps = jax.random.uniform(jax.random.fold_in(jax.random.fold_in(own_key, 6), position), (blocks,), jnp.float32, low / len(cuts), high / len(cuts))
        return jnp.repeat(jnp.exp(steps), shape[position] // blocks).reshape((-1,) + (1,) * (len(shape) - position - 1))

    loudness = one(*cuts[0])
    for cut in cuts[1:]:
        loudness = loudness * one(*cut)
    return loudness


def deal_out(rng, own, number, rows, number_of, top, limit, slope):
    ranking = jax.random.permutation(rng, number_of)
    packed, usual = load_shares(number_of, rows * top, limit, slope, True), load_shares(number_of, rows * top, limit, slope, False)
    places = jnp.arange(number_of)

    def named(sizes, offset_by):
        used = int((sizes > 0).sum())
        fixed = max(1, used // 4)
        shifted = fixed + (places - fixed + offset_by * (used - fixed)) % max(1, number_of - fixed)
        return jnp.zeros((number_of,), jnp.int32).at[ranking[jnp.where(places < fixed, places, shifted)]].set(jnp.asarray(sizes, jnp.int32))

    sizes = jnp.where(number % 4 == 0, named(packed, number // 4), named(usual, number - number // 4 - 1))
    mixed = jax.random.permutation(jax.random.fold_in(own, 3), number_of)
    donor, taker = mixed[0:number_of // 2 * 2:2], mixed[1:number_of // 2 * 2:2]
    room = jnp.minimum(sizes[donor] - 1, limit - sizes[taker]) // 2
    room = jnp.where((donor == ranking[0]) | (taker == ranking[0]) | (sizes[taker] == 0), 0, jnp.maximum(room, 0))
    shifted = jax.random.randint(jax.random.fold_in(own, 4), (number_of // 2,), 0, 1 << 20) % (room + 1)
    sizes = sizes.at[donor].add(-shifted).at[taker].add(shifted)
    labels = jnp.searchsorted(jnp.cumsum(sizes), jnp.arange(rows * top), side="right").astype(jnp.int32)
    listing = labels.reshape(top, rows).T
    listing = listing[jax.random.permutation(jax.random.fold_in(own, 1), rows)]
    offset_by = jax.random.randint(jax.random.fold_in(own, 2), (rows, 1), 0, top)
    return jnp.take_along_axis(listing, (jnp.arange(top)[None, :] + offset_by) % top, axis=1)


def load_shares(amount, total, most, lean, full):
    weights = [(1 << 20) // math.isqrt(grade ** lean) + 1 for grade in range(1, amount + 1)]
    largest = most if full else min(most, max(-(-total // amount), total * weights[0] // sum(weights)))
    least = 1 if total - largest >= amount - 1 else 0
    given, spare = [largest] + [least] * (amount - 1), total - largest - least * (amount - 1)
    while spare > 0:
        free = [i for i in range(1, amount) if given[i] < largest] or [i for i in range(1, amount) if given[i] < most]
        pool, left = sum([weights[i] for i in free]), spare
        for i in free:
            addition = min(most - given[i], max(1, left * weights[i] // pool), spare)
            given[i] = given[i] + addition
            spare = spare - addition
    return np.array(given)


def normal_values(key, shape, deviation, most, cuts=(), held_as=jnp.bfloat16):
    loudness = level_of(key, shape, cuts, -0.22, 0.18) if cuts else 1.0
    drawn = jax.random.normal(key, shape, jnp.float32) * deviation * loudness
    return jnp.minimum(jnp.maximum(drawn, -most), most).astype(held_as)


def setup_inputs(seed: int = 0) -> dict:
    key_of = jax.random.split(jax.random.key(seed), 15)
    queries = draw_queries(jax.random.fold_in(key_of[14], 71), 0)
    keys = draw_keys(jax.random.fold_in(key_of[14], 71), 0)
    values = normal_values(key_of[2], (SEQUENCE_TOKENS, KEY_VALUE_HEADS * HEAD_DIMENSION), 1.0, 6.0, ((0, 8), (1, 4)))
    query_gain = draw_query_gain(jax.random.fold_in(key_of[14], 71), 0)
    key_norm_gain = draw_key_norm_gain(jax.random.fold_in(key_of[14], 71), 0)
    attn_gain = jnp.clip(1.0 + 0.18 * jax.random.normal(key_of[5], (QUERY_HEADS * HEAD_DIMENSION,), jnp.float32), 0.1, 1.9)
    residual = draw_residual(jax.random.fold_in(key_of[14], 71), 0)
    out_weight = normal_values(key_of[7], (QUERY_HEADS * HEAD_DIMENSION, D), (QUERY_HEADS * HEAD_DIMENSION) ** -0.5, 0.1875, ((1, 4),))
    ffn_gain = jnp.clip(1.0 + 0.18 * jax.random.normal(key_of[8], (D,), jnp.float32), 0.1, 1.9)
    routes_keys = jax.random.split(jax.random.fold_in(key_of[9], 1), SEQUENCE_TOKENS // TOK_SP)
    routes_turns = jax.random.permutation(jax.random.fold_in(key_of[9], 3), SEQUENCE_TOKENS // TOK_SP)
    routes = jax.vmap(lambda own, number: deal_out(jax.random.fold_in(key_of[9], 2), own, number, TOK_SP, EXPERTS, TOPK, CAP, 2))(routes_keys, routes_turns).reshape((SEQUENCE_TOKENS, TOPK))
    route_weight = jnp.clip(0.2 + 0.8 * jax.random.uniform(key_of[10], (SEQUENCE_TOKENS, TOPK), jnp.float32) ** level_of(key_of[10], (SEQUENCE_TOKENS, TOPK), ((0, 8),), -0.2, 0.2), 0.2, 1.0)
    gate_weight = normal_values(key_of[11], (EXPERTS, D, FF), (D // 16) ** -0.5, 0.5, ((0, 8), (2, 4)))
    up_weight = normal_values(key_of[12], (EXPERTS, D, FF), (D // 16) ** -0.5, 0.5, ((0, 8), (2, 4)))
    down_weight = normal_values(key_of[13], (EXPERTS, FF, D), (FF * 400) ** -0.5, 0.0068359375, ((0, 8), (1, 4)))
    return dict(queries=queries, keys=keys, values=values, query_gain=query_gain, key_norm_gain=key_norm_gain, attn_gain=attn_gain, residual=residual, out_weight=out_weight, ffn_gain=ffn_gain, routes=routes, route_weight=route_weight, gate_weight=gate_weight, up_weight=up_weight, down_weight=down_weight)


EPS = 1e-06
THETA = 10000.0
ALPHA = 1.702
LIMIT = 7.0

def rotary_tables(positions, head_size, grid_width):
    row_pos = (positions // grid_width).astype(jnp.float32)
    col_pos = (positions % grid_width).astype(jnp.float32)
    half_size = head_size // 2
    inverse = THETA ** (-jnp.arange(0, half_size, 2, dtype=jnp.float32) / half_size)
    angles = jnp.concatenate([row_pos[:, None] * inverse, col_pos[:, None] * inverse], axis=-1)
    return (jnp.cos(angles), jnp.sin(angles))

def normalize_then_rotate(head_rows, gain_vector, cosine_lookup, sine_lookup):
    values_f = head_rows.astype(jnp.float32)
    scaled = values_f * lax.rsqrt(lax.optimization_barrier(jnp.mean(values_f * values_f, axis=-1, keepdims=True)) + EPS) * gain_vector
    first_half, second_half = jnp.split(scaled, 2, axis=-1)
    cos_part = cosine_lookup[:, None, :]
    sin_part = sine_lookup[:, None, :]
    return jnp.concatenate([first_half * cos_part - second_half * sin_part, first_half * sin_part + second_half * cos_part], axis=-1).astype(jnp.bfloat16)

def clamped_unit(gate_sum, up_sum):
    gate_sum = jnp.minimum(gate_sum, LIMIT)
    up_sum = jnp.clip(up_sum, -LIMIT, LIMIT)
    return ((up_sum + 1.0) * gate_sum * jax.nn.sigmoid(ALPHA * gate_sum)).astype(jnp.bfloat16)

def reference(queries, keys, values, query_gain, key_norm_gain, attn_gain, residual, out_weight, ffn_gain, routes, route_weight, gate_weight, up_weight, down_weight):
    group_width = QUERY_HEADS // KEY_VALUE_HEADS
    positions = jnp.arange(SEQUENCE_TOKENS, dtype=jnp.int32)
    cosine_lookup, sine_lookup = rotary_tables(positions, HEAD_DIMENSION, GRID_W)
    query_rotated = normalize_then_rotate(queries.reshape(SEQUENCE_TOKENS, QUERY_HEADS, HEAD_DIMENSION), query_gain, cosine_lookup, sine_lookup)
    query_rotated = query_rotated.reshape(SEQUENCE_TOKENS // 256, 256, KEY_VALUE_HEADS, group_width, HEAD_DIMENSION)
    key_rotated = normalize_then_rotate(keys.reshape(SEQUENCE_TOKENS, KEY_VALUE_HEADS, HEAD_DIMENSION), key_norm_gain, cosine_lookup, sine_lookup).astype(jnp.float32)
    value_float = values.reshape(SEQUENCE_TOKENS, KEY_VALUE_HEADS, HEAD_DIMENSION).astype(jnp.float32)

    def attend(query_block):
        query_f = query_block.astype(jnp.float32)
        scores = jnp.einsum('qkgd,nkd->kgqn', query_f, key_rotated) * HEAD_DIMENSION ** (-0.5)
        row_max = lax.optimization_barrier(jnp.max(scores, axis=-1, keepdims=True))
        weights = jnp.exp(scores - row_max)
        row_sum = lax.optimization_barrier(jnp.sum(weights, axis=-1))
        mixed = jnp.einsum('kgqn,nkd->qkgd', weights.astype(jnp.bfloat16).astype(jnp.float32), value_float)
        return mixed / jnp.transpose(row_sum, (2, 0, 1))[..., None]
    attended = lax.map(attend, query_rotated).reshape(SEQUENCE_TOKENS, QUERY_HEADS * HEAD_DIMENSION).astype(jnp.bfloat16)
    head_f = attended.astype(jnp.float32)
    attn_normed = (head_f * lax.rsqrt(lax.optimization_barrier(jnp.mean(head_f * head_f, axis=-1, keepdims=True)) + EPS) * attn_gain).astype(jnp.bfloat16)
    mid_stream = (residual.astype(jnp.float32) + jnp.dot(attn_normed, out_weight, preferred_element_type=jnp.float32)).astype(jnp.bfloat16)
    mid_f = mid_stream.astype(jnp.float32)
    ffn_in = (mid_f * lax.rsqrt(lax.optimization_barrier(jnp.mean(mid_f * mid_f, axis=-1, keepdims=True)) + EPS) * ffn_gain).astype(jnp.bfloat16)
    blocks = N_SP
    route_list = routes.reshape(blocks, TOK_SP * TOPK)
    onehot = (route_list[..., None] == jnp.arange(EXPERTS, dtype=jnp.int32)[None, None, :]).astype(jnp.int32)
    route_ranks = lax.optimization_barrier(jnp.sum((jnp.cumsum(onehot, axis=1) - 1) * onehot, axis=2))
    block_ids = jnp.arange(blocks, dtype=jnp.int32)[:, None]
    slot_index = (route_list * (blocks * CAP) + block_ids * CAP + route_ranks).reshape(-1)
    token_ids = (block_ids * TOK_SP + jnp.arange(TOK_SP * TOPK, dtype=jnp.int32)[None, :] // TOPK).reshape(-1)
    slot_owner = jnp.full((EXPERTS * blocks * CAP,), SEQUENCE_TOKENS, jnp.int32).at[slot_index].set(token_ids)
    padded = jnp.concatenate([ffn_in, jnp.zeros((1, D), jnp.bfloat16)], axis=0)
    dispatched = padded[slot_owner].reshape(EXPERTS, blocks * CAP, D)

    def expert(operands):
        slot_rows, w_gate, w_up, w_down = operands
        gate_sum = jnp.dot(slot_rows, w_gate, preferred_element_type=jnp.float32)
        up_sum = jnp.dot(slot_rows, w_up, preferred_element_type=jnp.float32)
        activation = clamped_unit(gate_sum, up_sum)
        parts = jnp.einsum('rjf,jfd->jrd', activation.reshape(-1, N_TP, FF // N_TP).astype(jnp.float32), w_down.reshape(N_TP, FF // N_TP, D).astype(jnp.float32))
        return lax.optimization_barrier(jnp.sum(parts.astype(jnp.bfloat16).astype(jnp.float32), axis=0)).astype(jnp.bfloat16)
    expert_out = lax.map(expert, (dispatched, gate_weight, up_weight, down_weight))
    picked = expert_out.reshape(-1, D)[slot_index].astype(jnp.float32)
    weighted = lax.optimization_barrier(jnp.sum((picked * route_weight.reshape(-1)[:, None]).reshape(SEQUENCE_TOKENS, TOPK, D), axis=1))
    return (mid_f + weighted).astype(jnp.bfloat16)
```

```python
import jax
import jax.numpy as jnp
from jax import lax
from jax.sharding import PartitionSpec as P

D = 2048
GRID_W = 64
CHUNKS = ((0, 1), (2, 3))


EPS = 1e-06
THETA = 10000.0
ALPHA = 1.702
LIMIT = 7.0


def rotary_tables(positions, head_size, grid_width):
    row_pos = (positions // grid_width).astype(jnp.float32)
    col_pos = (positions % grid_width).astype(jnp.float32)
    half_size = head_size // 2
    inverse = THETA ** (-jnp.arange(0, half_size, 2, dtype=jnp.float32) / half_size)
    angles = jnp.concatenate([row_pos[:, None] * inverse, col_pos[:, None] * inverse], axis=-1)
    return (jnp.cos(angles), jnp.sin(angles))


def normalize_then_rotate(head_rows, gain_vector, cosine_lookup, sine_lookup):
    values_f = head_rows.astype(jnp.float32)
    scaled = (
        values_f
        * lax.rsqrt(jnp.mean(values_f * values_f, axis=-1, keepdims=True) + EPS)
        * gain_vector
    )
    first_half, second_half = jnp.split(scaled, 2, axis=-1)
    cos_part = cosine_lookup[:, None, :]
    sin_part = sine_lookup[:, None, :]
    return jnp.concatenate(
        [
            first_half * cos_part - second_half * sin_part,
            first_half * sin_part + second_half * cos_part,
        ],
        axis=-1,
    ).astype(jnp.bfloat16)


def clamped_unit(gate_sum, up_sum):
    gate_sum = jnp.minimum(gate_sum, LIMIT)
    up_sum = jnp.clip(up_sum, -LIMIT, LIMIT)
    return ((up_sum + 1.0) * gate_sum * jax.nn.sigmoid(ALPHA * gate_sum)).astype(jnp.bfloat16)


def routed_path(
    queries,
    keys,
    values,
    query_gain,
    key_norm_gain,
    attn_gain,
    residual,
    out_weight,
    ffn_gain,
    routes,
    route_weight,
    gate_weight,
    up_weight,
    down_weight,
):
    tokens = queries.shape[0]
    head_size = query_gain.shape[0]
    kv_local = keys.shape[1] // head_size
    q_local = queries.shape[1] // head_size
    group_width = q_local // kv_local
    first_token = lax.axis_index("sp") * tokens
    positions = first_token + jnp.arange(tokens, dtype=jnp.int32)
    cosine_lookup, sine_lookup = rotary_tables(positions, head_size, GRID_W)
    query_rotated = normalize_then_rotate(
        queries.reshape(tokens, q_local, head_size), query_gain, cosine_lookup, sine_lookup
    )
    key_rotated = normalize_then_rotate(
        keys.reshape(tokens, kv_local, head_size), key_norm_gain, cosine_lookup, sine_lookup
    )
    query_rows = query_rotated.reshape(tokens, kv_local, group_width, head_size).transpose(
        1, 0, 2, 3
    )
    query_rows = query_rows.reshape(kv_local, tokens * group_width, head_size)
    value_rows = values.reshape(tokens, kv_local, head_size)
    score_scale = head_size ** (-0.5)
    query_width = tokens * group_width
    start_state = (
        jnp.full((kv_local, query_width), -1e30, jnp.float32),
        jnp.zeros((kv_local, query_width), jnp.float32),
        jnp.zeros((kv_local, query_width, head_size), jnp.float32),
    )
    piece_keys = lax.all_gather(key_rotated, "sp", axis=0, tiled=True)
    piece_values = lax.all_gather(value_rows, "sp", axis=0, tiled=True)
    slot_count = piece_keys.shape[0]
    block_rows = 2048
    key_blocks = piece_keys.reshape(slot_count // block_rows, block_rows, kv_local, head_size)
    value_blocks = piece_values.reshape(slot_count // block_rows, block_rows, kv_local, head_size)

    def one_block(softmax_state, pair_block):
        running_max, running_sum, accumulated = softmax_state
        key_block, value_block = pair_block
        scores = (
            jnp.einsum("kqd,nkd->kqn", query_rows, key_block, preferred_element_type=jnp.float32)
            * score_scale
        )
        new_max = jnp.maximum(running_max, jnp.max(scores, axis=-1))
        weights = jnp.exp(scores - new_max[..., None])
        factor = jnp.exp(running_max - new_max)
        running_sum = running_sum * factor + jnp.sum(weights, axis=-1)
        accumulated = accumulated * factor[..., None] + jnp.einsum(
            "kqn,nkd->kqd",
            weights.astype(jnp.bfloat16),
            value_block,
            preferred_element_type=jnp.float32,
        )
        return ((new_max, running_sum, accumulated), None)

    final_state, unused_out = lax.scan(one_block, start_state, (key_blocks, value_blocks))
    running_max, running_sum, accumulated = final_state
    attended = (accumulated / running_sum[..., None]).reshape(
        kv_local, tokens, group_width, head_size
    )
    attended = (
        attended.transpose(1, 0, 2, 3).reshape(tokens, q_local * head_size).astype(jnp.bfloat16)
    )
    all_heads = lax.all_gather(attended, "tp", axis=1, tiled=True)
    head_f = all_heads.astype(jnp.float32)
    attn_normed = (
        head_f * lax.rsqrt(jnp.mean(head_f * head_f, axis=-1, keepdims=True) + EPS) * attn_gain
    ).astype(jnp.bfloat16)
    mid_stream = (
        residual.astype(jnp.float32)
        + jnp.dot(attn_normed, out_weight, preferred_element_type=jnp.float32)
    ).astype(jnp.bfloat16)
    mid_f = mid_stream.astype(jnp.float32)
    square_total = lax.psum(jnp.sum(mid_f * mid_f, axis=-1), "tp")
    ffn_in = (mid_f * lax.rsqrt(square_total / D + EPS)[:, None] * ffn_gain).astype(jnp.bfloat16)
    experts = lax.axis_size("sp")
    top_k = routes.shape[1]
    capacity = tokens * top_k * 3 // (2 * experts)
    route_list = routes.reshape(-1)
    onehot = (route_list[:, None] == jnp.arange(experts, dtype=jnp.int32)[None, :]).astype(
        jnp.int32
    )
    route_ranks = jnp.sum((jnp.cumsum(onehot, axis=0) - 1) * onehot, axis=1)
    slot_index = route_list * capacity + route_ranks
    slot_owner = (
        jnp.full((experts * capacity,), tokens, jnp.int32)
        .at[slot_index]
        .set(jnp.arange(tokens * top_k, dtype=jnp.int32) // top_k)
    )
    padded = jnp.concatenate([ffn_in, jnp.zeros((1, ffn_in.shape[1]), ffn_in.dtype)], axis=0)
    slot_block = lax.all_to_all(
        padded[slot_owner].reshape(experts, capacity, ffn_in.shape[1]),
        "sp",
        split_axis=0,
        concat_axis=0,
        tiled=True,
    )
    slot_count = slot_block.shape[1]
    slot_rows = slot_block.reshape(-1, slot_block.shape[2])
    column_piece = lax.all_gather(slot_rows, "tp", axis=1, tiled=True)
    gate_rows = gate_weight[0]
    up_rows = up_weight[0]
    gate_sum = jnp.dot(column_piece, gate_rows, preferred_element_type=jnp.float32)
    up_sum = jnp.dot(column_piece, up_rows, preferred_element_type=jnp.float32)
    partial_value = jnp.dot(
        clamped_unit(gate_sum, up_sum), down_weight[0], preferred_element_type=jnp.float32
    )
    summed = lax.psum_scatter(
        partial_value.astype(jnp.bfloat16), "tp", scatter_dimension=1, tiled=True
    )
    results = lax.all_to_all(
        summed.reshape(experts, slot_count, summed.shape[1]),
        "sp",
        split_axis=0,
        concat_axis=0,
        tiled=True,
    )
    picked = results.reshape(experts * capacity, -1)[slot_index].astype(jnp.float32)
    weighted = jnp.sum(
        (picked * route_weight.reshape(-1)[:, None]).reshape(tokens, top_k, -1), axis=1
    )
    return (mid_f + weighted).astype(jnp.bfloat16)


def joint_pairs(n_sp, n_tp, move):
    pairs = []
    for sp in range(n_sp):
        for tp in range(n_tp):
            to_sp, to_tp = move(sp, tp)
            pairs.append((sp * n_tp + tp, to_sp * n_tp + to_tp))
    return pairs


def dense_path(
    n_sp,
    n_tp,
    chunks,
    queries,
    keys,
    values,
    query_gain,
    key_norm_gain,
    attn_gain,
    residual,
    out_weight,
    ffn_gain,
    routes,
    route_weight,
    gate_weight,
    up_weight,
    down_weight,
):
    both = ("sp", "tp")

    def mover(move):
        pairs = joint_pairs(n_sp, n_tp, move)
        return lambda array: lax.ppermute(array, both, pairs)

    to_core = mover(lambda sp, tp: (sp, tp ^ 1))
    to_x = mover(lambda sp, tp: (sp, tp ^ 2))
    to_y = mover(lambda sp, tp: (sp ^ 1, tp))
    to_z = [mover(lambda sp, tp, d=d: (sp ^ (2 * d), tp)) for d in range(n_sp // 2)]
    to_yx = mover(lambda sp, tp: (sp ^ 1, tp) if tp % 2 == 0 else (sp, tp ^ 2))
    to_xy = mover(lambda sp, tp: (sp, tp ^ 2) if tp % 2 == 0 else (sp ^ 1, tp))

    expert = lax.axis_index("sp")
    place = lax.axis_index("tp")
    core = place % 2
    first_core = core == 0
    tokens = queries.shape[0]
    half = tokens // 2
    quarter = residual.shape[1]
    model = quarter * n_tp

    def halves(array):
        mine = lax.dynamic_slice_in_dim(array, core * half, half, 0)
        other = lax.dynamic_slice_in_dim(array, (1 - core) * half, half, 0)
        return mine, other

    def split_tokens(array):
        mine, other = halves(array)
        return jnp.concatenate([mine, to_core(other)], axis=1)

    def own_first(array, axis, count):
        size = array.shape[axis] // n_tp
        return jnp.concatenate(
            [
                lax.dynamic_slice_in_dim(array, (place ^ k) * size, size, axis)
                for k in range(count)
            ],
            axis=axis,
        )

    head_size = query_gain.shape[0]
    kv_local = keys.shape[1] // head_size
    q_local = queries.shape[1] // head_size
    group_width = q_local // kv_local
    positions = expert * tokens + jnp.arange(tokens, dtype=jnp.int32)
    cosine_lookup, sine_lookup = rotary_tables(positions, head_size, GRID_W)
    key_rotated = normalize_then_rotate(
        keys.reshape(tokens, kv_local, head_size), key_norm_gain, cosine_lookup, sine_lookup
    ).reshape(tokens, kv_local * head_size)
    named = routes.T[None] == jnp.arange(n_sp, dtype=jnp.int32)[:, None, None]
    share = jnp.sum(jnp.where(named, route_weight.T[None], 0.0), axis=1)
    high = lax.reduce_precision(share, 8, 7)
    middle = lax.reduce_precision(share - high, 8, 7)
    low = share - high - middle
    width = 2 * kv_local * head_size
    share_rows = jnp.stack([high, middle, low]).astype(jnp.bfloat16).reshape(-1, width)
    share_count = share_rows.shape[0]
    packet = jnp.concatenate(
        [jnp.concatenate([key_rotated, values], axis=1), share_rows], axis=0
    )
    packets = jnp.stack([packet] + [to_z[d](packet) for d in range(1, n_sp // 2)])
    packets = jnp.stack([packets, to_y(packets)])

    all_kv = packets[:, :, :tokens].reshape(n_sp * tokens, width)
    all_keys = all_kv[:, : width // 2].reshape(n_sp * tokens, kv_local, head_size)
    all_values = all_kv[:, width // 2 :].reshape(n_sp * tokens, kv_local, head_size)
    shares = packets[:, :, tokens:].reshape(2, n_sp // 2, 3, n_sp, tokens).astype(jnp.float32)
    shares = lax.dynamic_index_in_dim(shares, expert, 3, keepdims=False)
    shares = lax.dynamic_slice_in_dim(shares, core * half, half, 3)
    shares = shares[:, :, 0] + shares[:, :, 1] + shares[:, :, 2]

    query_rotated = normalize_then_rotate(
        queries.reshape(tokens, q_local, head_size), query_gain, cosine_lookup, sine_lookup
    )
    query_rows = query_rotated.reshape(tokens, kv_local, group_width, head_size)
    query_rows = query_rows.transpose(1, 0, 2, 3).reshape(kv_local, -1, head_size)
    scores = jnp.einsum("kqd,nkd->kqn", query_rows, all_keys, preferred_element_type=jnp.float32)
    scores = scores * head_size ** (-0.5)
    weights = jnp.exp(scores - jnp.max(scores, axis=-1, keepdims=True))
    attended = jnp.einsum(
        "kqn,nkd->kqd",
        weights.astype(jnp.bfloat16),
        all_values,
        preferred_element_type=jnp.float32,
    )
    attended = attended / jnp.sum(weights, axis=-1)[..., None]
    attended = attended.reshape(kv_local, tokens, group_width, head_size).transpose(1, 0, 2, 3)
    attended = attended.reshape(tokens, q_local * head_size).astype(jnp.bfloat16)

    chip_heads = split_tokens(attended)
    head_f = jnp.concatenate([chip_heads, to_x(chip_heads)], axis=1).astype(jnp.float32)
    attn_normed = (
        head_f
        * lax.rsqrt(jnp.mean(head_f * head_f, axis=-1, keepdims=True) + EPS)
        * own_first(attn_gain, 0, n_tp)
    ).astype(jnp.bfloat16)
    chip_out = jnp.concatenate([out_weight, to_core(out_weight)], axis=1)
    mid_f = split_tokens(residual).astype(jnp.float32) + jnp.dot(
        attn_normed, own_first(chip_out, 0, n_tp), preferred_element_type=jnp.float32
    )
    mid_stream = mid_f.astype(jnp.bfloat16)
    chip_width = mid_stream.shape[1]

    gains = jnp.concatenate([ffn_gain, to_core(ffn_gain)])
    gains = jnp.concatenate([gains, to_x(gains)])
    gate = own_first(jnp.concatenate([gate_weight[0], to_core(gate_weight[0])], axis=1), 0, n_tp)
    up = own_first(jnp.concatenate([up_weight[0], to_core(up_weight[0])], axis=1), 0, n_tp)
    down = own_first(
        jnp.concatenate([down_weight[0], to_core(down_weight[0])], axis=0), 1, n_tp
    )

    def spread(blocks):
        from_x = to_x(blocks)
        from_y = to_y(blocks)
        corner = to_yx(jnp.where(first_core, from_x, from_y))
        return jnp.concatenate(
            [
                jnp.concatenate([blocks, from_x], axis=-1)[None],
                jnp.concatenate([from_y, corner], axis=-1)[None],
            ]
        )

    def feed(rows, share):
        shape = rows.shape
        rows_f = rows.reshape(-1, model).astype(jnp.float32)
        ffn_in = (
            rows_f * lax.rsqrt(jnp.mean(rows_f * rows_f, axis=-1, keepdims=True) + EPS) * gains
        ).astype(jnp.bfloat16)
        gate_sum = jnp.dot(ffn_in, gate, preferred_element_type=jnp.float32)
        up_sum = jnp.dot(ffn_in, up, preferred_element_type=jnp.float32)
        partial = jnp.dot(
            clamped_unit(gate_sum, up_sum), down, preferred_element_type=jnp.float32
        )
        return (partial * share.reshape(-1, 1)).astype(jnp.bfloat16).reshape(shape)

    def collect(partial):
        mine, other = partial[0], partial[1]
        b00, b01 = mine[..., :chip_width], mine[..., chip_width:]
        b10, b11 = other[..., :chip_width], other[..., chip_width:]
        arrived = to_yx(jnp.stack([jnp.where(first_core, b10, b01), b11])).astype(jnp.float32)
        kept = jnp.where(first_core, b01, b10).astype(jnp.float32)
        last = to_xy((kept + arrived[1]).astype(jnp.bfloat16)).astype(jnp.float32)
        return b00.astype(jnp.float32) + arrived[0] + last

    weighted = jnp.zeros((half, chip_width), jnp.float32)
    for chunk in chunks:
        blocks = jnp.stack([mid_stream if d == 0 else to_z[d](mid_stream) for d in chunk])
        share = jnp.stack([shares[:, d] for d in chunk], axis=1)
        sums = collect(feed(spread(blocks), share))
        for i, d in enumerate(chunk):
            if d == 0:
                weighted = weighted + sums[i]
            else:
                weighted = weighted + to_z[d](sums[i].astype(jnp.bfloat16)).astype(jnp.float32)

    layer_out = (mid_stream.astype(jnp.float32) + weighted).astype(jnp.bfloat16)
    mine = layer_out[:, :quarter]
    theirs = to_core(layer_out[:, quarter:])
    return jnp.concatenate(
        [jnp.where(first_core, mine, theirs), jnp.where(first_core, theirs, mine)], axis=0
    )


def solution(mesh):
    placed = (
        P("sp", "tp"),
        P("sp", "tp"),
        P("sp", "tp"),
        P(),
        P(),
        P(),
        P("sp", "tp"),
        P(None, "tp"),
        P("tp"),
        P("sp", None),
        P("sp", None),
        P("sp", None, "tp"),
        P("sp", None, "tp"),
        P("sp", "tp", None),
    )
    n_sp, n_tp = mesh.shape["sp"], mesh.shape["tp"]

    def per_device(*arrays):
        tokens, top_k = arrays[9].shape
        capacity = tokens * top_k * 3 // (2 * n_sp)
        if 2 * capacity < tokens or n_tp != 4:
            return routed_path(*arrays)
        return dense_path(n_sp, n_tp, CHUNKS, *arrays)

    return jax.shard_map(
        per_device, mesh=mesh, in_specs=placed, out_specs=P("sp", "tp"), check_vma=False
    )
```
